32 devices in a mesh: sp: 8 (over z, x), tp: 4 (over y, core).
Axes of the slice: x: 2, y: 2, z: 4, core: 2. Of those that a mesh axis runs over, the one named last changes fastest.
Arguments:
- stream_in: bfloat16 [2048, 2048], P(('sp', 'tp')), may hold values from -6 to 6
- pre_gate: bfloat16 [2048, 1024], P('sp', 'tp'), may hold values from -6 to 6
- value_in: bfloat16 [2048, 1024], P('sp', 'tp'), may hold values from -6 to 6
- post_gate: bfloat16 [2048, 1024], P('sp', 'tp'), may hold values from -6 to 6
- conv_taps: bfloat16 [3, 1024], P(None, 'tp'), may hold values from -3 to 3
- out_weight: bfloat16 [1024, 2048], P('tp'), may hold values from -0.1875 to 0.1875
- route_ids: int32 [2048, 4], P('sp'), may hold values from 0 to 7, all different within a row; in each aligned block of 64 rows (0 to 63, 64 to 127, ...) at most 64 rows name the same one
- route_weight: float32 [2048, 4], P('sp'), may hold values from 0.1 to 1
- ffn_gain: bfloat16 [2048], replicated, may hold values from 0.099609375 to 1.8984375
- post_gain: bfloat16 [2048], replicated, may hold values from 0.099609375 to 1.8984375
- gate_proj: bfloat16 [8, 2048, 2048], P('sp', None, 'tp'), may hold values from -0.39648438 to 0.39648438
- up_proj: bfloat16 [8, 2048, 2048], P('sp', None, 'tp'), may hold values from -0.39648438 to 0.39648438
- down_proj: bfloat16 [8, 2048, 2048], P('sp', None, 'tp'), may hold values from -0.125 to 0.125
Outputs:
- layer_out: bfloat16 [2048, 2048], P(('sp', 'tp'))
The draws below stay inside these ranges and needn't reach their ends.
Inputs may be any that keep to these rules, and one draw needn't show every extreme that they name: `route_ids`: in each aligned block of 64 positions, a row names 4 different experts and no expert is named by more than 64 rows; in every draw some expert reaches 64 in some block.
All inputs are finite; a program needn't handle non-finite values.
Results may differ from the reference program's by a relative error of at most 0.014.
Values may be sent and summed in bfloat16 or wider, within the bound.
No kernel may reach another device: no remote copies, remote signals or barrier semaphores. Data moves between devices by JAX's collectives and lax.ppermute only.
A program may use at most 64 MiB of HBM per device.

```python
import math
import jax
import jax.numpy as jnp
import numpy as np
from jax import lax

D = 2048
W = 1024
FF = 2048
TOPK = 4
KERNEL = 3
TOKENS = 2048
EXPERTS = 8
ROWS = 64
CAP = 64
SLOTS = 2048


def shard_levels(key, extent, shards, low, top_value):
    level, own = 1.0, jax.random.fold_in(key, 6)
    for position, blocks in shards:
        heights = jnp.exp(jax.random.uniform(jax.random.fold_in(own, position), (blocks,), jnp.float32, low / len(shards), top_value / len(shards)))
        level = level * jnp.repeat(heights, extent[position] // blocks).reshape([-1 if axis == position else 1 for axis in range(len(extent))])
    return level


def deal_out(stream_key, own, number, rows, count, top, bound, slope):
    sequence = jax.random.permutation(stream_key, count)
    crowded, ordinary = load_shares(count, rows * top, bound, slope, True), load_shares(count, rows * top, bound, slope, False)
    places = jnp.arange(count)

    def named(lengths, rotation):
        used = int((lengths > 0).sum())
        fixed = max(1, used // 4)
        moved = fixed + (places - fixed + rotation * (used - fixed)) % max(1, count - fixed)
        return jnp.zeros((count,), jnp.int32).at[sequence[jnp.where(places < fixed, places, moved)]].set(jnp.asarray(lengths, jnp.int32))

    lengths = jnp.where(number % 4 == 0, named(crowded, number // 4), named(ordinary, number - number // 4 - 1))
    mixed = jax.random.permutation(jax.random.fold_in(own, 3), count)
    donor, receiver = mixed[0:count // 2 * 2:2], mixed[1:count // 2 * 2:2]
    margin = jnp.minimum(lengths[donor] - 1, bound - lengths[receiver]) // 2
    margin = jnp.where((donor == sequence[0]) | (receiver == sequence[0]) | (lengths[receiver] == 0), 0, jnp.maximum(margin, 0))
    moved = jax.random.randint(jax.random.fold_in(own, 4), (count // 2,), 0, 1 << 20) % (margin + 1)
    lengths = lengths.at[donor].add(-moved).at[receiver].add(moved)
    members = jnp.searchsorted(jnp.cumsum(lengths), jnp.arange(rows * top), side="right").astype(jnp.int32)
    grid = members.reshape(top, rows).T
    grid = grid[jax.random.permutation(jax.random.fold_in(own, 1), rows)]
    rotation = jax.random.randint(jax.random.fold_in(own, 2), (rows, 1), 0, top)
    return jnp.take_along_axis(grid, (jnp.arange(top)[None, :] + rotation) % top, axis=1)


def load_shares(number_of, total, bound, lean, full):
    portions = [(1 << 20) // math.isqrt(standing ** lean) + 1 for standing in range(1, number_of + 1)]
    largest = bound if full else min(bound, max(-(-total // number_of), total * portions[0] // sum(portions)))
    least = 1 if total - largest >= number_of - 1 else 0
    counts, rest = [largest] + [least] * (number_of - 1), total - largest - least * (number_of - 1)
    while rest > 0:
        candidates = [i for i in range(1, number_of) if counts[i] < largest] or [i for i in range(1, number_of) if counts[i] < bound]
        whole, remaining = sum([portions[i] for i in candidates]), rest
        for i in candidates:
            addition = min(bound - counts[i], max(1, remaining * portions[i] // whole), rest)
            counts[i] = counts[i] + addition
            rest = rest - addition
    return np.array(counts)


def normal_values(rng, extent, width, limit, split=(), kind=jnp.bfloat16):
    drawn = width * jax.random.normal(rng, extent, jnp.float32)
    if split:
        drawn = drawn * shard_levels(rng, extent, split, -0.22, 0.18)
    return jnp.clip(drawn, -limit, limit).astype(kind)


def setup_inputs(seed: int = 0) -> dict:
    key_of = jax.random.split(jax.random.key(seed), 14)
    stream_in = normal_values(key_of[0], (TOKENS, D), 1.0, 6.0, ((0, 32),))
    pre_gate = normal_values(key_of[1], (TOKENS, W), 1.0, 6.0, ((0, 8), (1, 4)))
    value_in = normal_values(key_of[2], (TOKENS, W), 1.0, 6.0, ((0, 8), (1, 4)))
    post_gate = normal_values(key_of[3], (TOKENS, W), 1.0, 6.0, ((0, 8), (1, 4)))
    conv_taps = normal_values(key_of[4], (KERNEL, W), 0.6, 3.0, ((1, 4),))
    out_weight = normal_values(key_of[5], (W, D), W ** -0.5, 0.1875, ((0, 4),))
    route_ids_keys = jax.random.split(jax.random.fold_in(key_of[6], 1), TOKENS // ROWS)
    route_ids_turns = jax.random.permutation(jax.random.fold_in(key_of[6], 3), TOKENS // ROWS)
    route_ids = jax.vmap(lambda own, number: deal_out(jax.random.fold_in(key_of[6], 2), own, number, ROWS, EXPERTS, TOPK, CAP, 2))(route_ids_keys, route_ids_turns).reshape((TOKENS, TOPK))
    route_weight = jnp.clip(jnp.exp(math.log(1.0) - 2.3025851 * jax.random.uniform(key_of[7], (TOKENS, TOPK), jnp.float32) ** shard_levels(key_of[7], (TOKENS, TOPK), ((0, 8),), -0.2, 0.2)), 0.1, 1.0)
    ffn_gain = jnp.clip(1.0 + 0.18 * jax.random.normal(key_of[8], (D,), jnp.float32), 0.099609375, 1.8984375).astype(jnp.bfloat16)
    post_gain = jnp.clip(1.0 + 0.18 * jax.random.normal(key_of[9], (D,), jnp.float32), 0.099609375, 1.8984375).astype(jnp.bfloat16)
    gate_proj = normal_values(key_of[10], (EXPERTS, D, FF), (3.0 * D ** -0.5), 0.39648438, ((0, 8), (2, 4)))
    up_proj = normal_values(key_of[11], (EXPERTS, D, FF), (3.0 * D ** -0.5), 0.39648438, ((0, 8), (2, 4)))
    down_proj = normal_values(key_of[12], (EXPERTS, FF, D), FF ** -0.5, 0.125, ((0, 8), (2, 4)))
    return dict(stream_in=stream_in, pre_gate=pre_gate, value_in=value_in, post_gate=post_gate, conv_taps=conv_taps, out_weight=out_weight, route_ids=route_ids, route_weight=route_weight, ffn_gain=ffn_gain, post_gain=post_gain, gate_proj=gate_proj, up_proj=up_proj, down_proj=down_proj)


clamp_limit = 7.0
sigmoid_scale = 1.702
epsilon = 1e-06

def clamped_units(gate_pre, up_pre):
    gate_cut = jnp.minimum(gate_pre, clamp_limit)
    up_cut = jnp.clip(up_pre, -clamp_limit, clamp_limit)
    return (up_cut + 1.0) * (gate_cut * jax.nn.sigmoid(sigmoid_scale * gate_cut))

def scaled_norm(values, gain):
    return values * lax.rsqrt(lax.optimization_barrier(jnp.mean(values * values, axis=-1, keepdims=True)) + epsilon) * gain.astype(jnp.float32)

def reference(stream_in, pre_gate, value_in, post_gate, conv_taps, out_weight, route_ids, route_weight, ffn_gain, post_gain, gate_proj, up_proj, down_proj):
    tap_count = conv_taps.shape[0]
    gated_input = (pre_gate.astype(jnp.float32) * value_in.astype(jnp.float32)).astype(jnp.bfloat16)
    padded = jnp.concatenate([jnp.zeros((tap_count - 1, W), jnp.bfloat16), gated_input], 0).astype(jnp.float32)
    convolved = jnp.zeros((TOKENS, W), jnp.float32)
    for tap_index in range(tap_count):
        convolved = convolved + conv_taps[tap_index].astype(jnp.float32)[None, :] * padded[tap_index:tap_index + TOKENS]
    mixer_out = (post_gate.astype(jnp.float32) * convolved).astype(jnp.bfloat16)
    projected = jnp.dot(mixer_out, out_weight, preferred_element_type=jnp.float32)
    residual = (stream_in.astype(jnp.float32) + projected).astype(jnp.bfloat16)
    normed = scaled_norm(residual.astype(jnp.float32), ffn_gain).astype(jnp.bfloat16)
    flattened = route_ids.reshape(-1).astype(jnp.int32)
    entries = flattened.shape[0]
    onehot = (flattened[:, None] == jnp.arange(EXPERTS, dtype=jnp.int32)[None, :]).astype(jnp.int32)
    blocked = onehot.reshape(entries // (ROWS * TOPK), ROWS * TOPK, EXPERTS)
    before = jnp.cumsum(blocked, axis=1) - blocked
    slot_rank = lax.optimization_barrier(jnp.sum(before * blocked, axis=2)).reshape(entries)
    block_ids = jnp.arange(entries, dtype=jnp.int32) // (ROWS * TOPK)
    slot_index = (block_ids * CAP + slot_rank).astype(jnp.int32)
    token_ids = jnp.arange(entries, dtype=jnp.int32) // TOPK
    slot_table = jnp.full((EXPERTS, SLOTS), TOKENS, jnp.int32).at[flattened, slot_index].set(token_ids)
    padded_rows = jnp.concatenate([normed, jnp.zeros((1, D), jnp.bfloat16)], 0)

    def one_expert(packed):
        token_rows, gate_matrix, up_matrix, down_matrix = packed
        inputs = padded_rows[token_rows]
        gate_pre = jnp.dot(inputs, gate_matrix, preferred_element_type=jnp.float32)
        up_pre = jnp.dot(inputs, up_matrix, preferred_element_type=jnp.float32)
        hidden = clamped_units(gate_pre, up_pre).astype(jnp.bfloat16)
        return jnp.dot(hidden, down_matrix, preferred_element_type=jnp.float32).astype(jnp.bfloat16)
    expert_outs = lax.map(one_expert, (slot_table, gate_proj, up_proj, down_proj))
    picked = expert_outs[flattened, slot_index].astype(jnp.float32).reshape(TOKENS, TOPK, D)
    combined = lax.optimization_barrier(jnp.sum(picked * route_weight[:, :, None], axis=1)).astype(jnp.bfloat16)
    layer_out = residual.astype(jnp.float32) + scaled_norm(combined.astype(jnp.float32), post_gain)
    return layer_out.astype(jnp.bfloat16)
```

```python
import jax
import jax.numpy as jnp
from jax import lax
from jax.sharding import PartitionSpec as P

clamp_limit = 7.0
sigmoid_scale = 1.702
epsilon = 1e-06


def passed_along(array, axis, by):
    count = lax.axis_size(axis)
    pairs = [(i, i + by) for i in range(count) if 0 <= i + by < count]
    return lax.ppermute(array, axis, pairs)


def clamped_units(gate_pre, up_pre):
    gate_cut = jnp.minimum(gate_pre, clamp_limit)
    up_cut = jnp.clip(up_pre, -clamp_limit, clamp_limit)
    return (up_cut + 1.0) * (gate_cut * jax.nn.sigmoid(sigmoid_scale * gate_cut))


def scaled_norm(values, gain):
    return (
        values
        * lax.rsqrt(jnp.mean(values * values, axis=-1, keepdims=True) + epsilon)
        * gain.astype(jnp.float32)
    )


def block_ranks(route_rows, experts, block_rows):
    flattened = route_rows.reshape(-1)
    entries = flattened.shape[0]
    span_width = block_rows * route_rows.shape[1]
    onehot = (flattened[:, None] == jnp.arange(experts, dtype=jnp.int32)[None, :]).astype(jnp.int32)
    blocked = onehot.reshape(entries // span_width, span_width, experts)
    before = jnp.cumsum(blocked, axis=1) - blocked
    return jnp.sum(before * blocked, axis=2).reshape(route_rows.shape)


def slot_picker(slot_index, table_size):
    matches = slot_index[None, :, :] == jnp.arange(table_size, dtype=jnp.int32)[:, None, None]
    return jnp.any(matches, axis=2).astype(jnp.bfloat16)


def mixed_rows(pre_gate, value_in, post_gate, conv_taps):
    seq_rows = pre_gate.shape[0]
    tap_count = conv_taps.shape[0]
    gated_input = (pre_gate.astype(jnp.float32) * value_in.astype(jnp.float32)).astype(jnp.bfloat16)
    rim_rows = passed_along(gated_input[seq_rows - tap_count + 1 :], "sp", 1)
    padded = jnp.concatenate([rim_rows, gated_input], 0).astype(jnp.float32)
    convolved = jnp.zeros(gated_input.shape, jnp.float32)
    for tap_index in range(tap_count):
        convolved = (
            convolved
            + conv_taps[tap_index].astype(jnp.float32)[None, :]
            * padded[tap_index : tap_index + seq_rows]
        )
    return (post_gate.astype(jnp.float32) * convolved).astype(jnp.bfloat16)


def slotted(
    stream_in,
    pre_gate,
    value_in,
    post_gate,
    conv_taps,
    out_weight,
    route_ids,
    route_weight,
    ffn_gain,
    post_gain,
    gate_proj,
    up_proj,
    down_proj,
):
    sp_count = lax.axis_size("sp")
    tp_count = lax.axis_size("tp")
    seq_rows = pre_gate.shape[0]
    own_rows = seq_rows // tp_count
    top_count = route_ids.shape[1]
    slots_each = 2 * own_rows * top_count // sp_count
    mixer_out = mixed_rows(pre_gate, value_in, post_gate, conv_taps)
    projected = lax.psum_scatter(
        jnp.dot(mixer_out, out_weight, preferred_element_type=jnp.float32),
        "tp",
        scatter_dimension=0,
        tiled=True,
    )
    residual = (stream_in.astype(jnp.float32) + projected).astype(jnp.bfloat16)
    normed = scaled_norm(residual.astype(jnp.float32), ffn_gain).astype(jnp.bfloat16)
    slot_rank = block_ranks(route_ids, sp_count, own_rows)
    block_of = (jnp.arange(seq_rows, dtype=jnp.int32) // own_rows)[:, None]
    tp_index = lax.axis_index("tp")
    own_ids = lax.dynamic_slice_in_dim(route_ids, tp_index * own_rows, own_rows, 0)
    own_rank = lax.dynamic_slice_in_dim(slot_rank, tp_index * own_rows, own_rows, 0)
    own_slot = own_ids * slots_each + own_rank
    picker = slot_picker(own_slot, sp_count * slots_each)
    outgoing = jnp.dot(picker, normed, preferred_element_type=jnp.float32).astype(jnp.bfloat16)
    arrived = lax.all_to_all(outgoing, "sp", split_axis=0, concat_axis=0, tiled=True)
    portion = lax.all_gather(arrived, "tp", axis=0, tiled=True)
    gate_pre = jnp.dot(portion, gate_proj[0], preferred_element_type=jnp.float32)
    up_pre = jnp.dot(portion, up_proj[0], preferred_element_type=jnp.float32)
    hidden = clamped_units(gate_pre, up_pre).astype(jnp.bfloat16)
    column_out = jnp.dot(
        lax.all_gather(hidden, "tp", axis=1, tiled=True),
        down_proj[0],
        preferred_element_type=jnp.float32,
    ).astype(jnp.bfloat16)
    column_width = column_out.shape[1]
    returned = lax.all_to_all(
        column_out.reshape(tp_count, sp_count, slots_each, column_width),
        "sp",
        split_axis=1,
        concat_axis=1,
        tiled=True,
    )
    home_index = (block_of * sp_count + route_ids) * slots_each + slot_rank
    gathered_out = jnp.take(returned.reshape(-1, column_width), home_index.reshape(-1), axis=0)
    gathered_out = gathered_out.astype(jnp.float32).reshape(seq_rows, top_count, column_width)
    combined_cols = jnp.sum(gathered_out * route_weight[:, :, None], axis=1).astype(jnp.bfloat16)
    combined = lax.all_to_all(combined_cols, "tp", split_axis=0, concat_axis=1, tiled=True)
    layer_out = residual.astype(jnp.float32) + scaled_norm(combined.astype(jnp.float32), post_gain)
    return layer_out.astype(jnp.bfloat16)


def dense(
    stream_in,
    pre_gate,
    value_in,
    post_gate,
    conv_taps,
    out_weight,
    route_ids,
    route_weight,
    ffn_gain,
    post_gain,
    gate_proj,
    up_proj,
    down_proj,
):
    sp_count = lax.axis_size("sp")
    tp_count = lax.axis_size("tp")
    sp_index = lax.axis_index("sp")
    tp_index = lax.axis_index("tp")
    seq_rows = pre_gate.shape[0]
    own_rows = seq_rows // tp_count
    half = own_rows // 2
    width = stream_in.shape[1]
    f32, bf16 = jnp.float32, jnp.bfloat16

    def swap(array, ds, dt):
        pairs = [
            (s * tp_count + t, (s ^ ds) * tp_count + (t ^ dt))
            for s in range(sp_count)
            for t in range(tp_count)
        ]
        return lax.ppermute(array, ("sp", "tp"), pairs)

    def core(array):
        return swap(array, 0, 1)

    def along_y(array):
        return swap(array, 0, 2)

    def along_x(array):
        return swap(array, 1, 0)

    def pieces(array, axis=0):
        size = array.shape[axis] // tp_count
        return [
            lax.dynamic_slice_in_dim(array, (tp_index ^ j) * size, size, axis)
            for j in range(tp_count)
        ]

    def y_turned(array):
        mid = array.shape[-1] // 2
        return jnp.concatenate([array[..., mid:], array[..., :mid]], axis=-1)

    gate_own, up_own = gate_proj[0], up_proj[0]
    gate_other, up_other = core(gate_own), core(up_own)
    down = pieces(down_proj[0])
    down_y = along_y(jnp.concatenate([down[2], down[3]], 0))
    hid = down[0].shape[0]
    down_c = core(jnp.concatenate([down[1], down[0]], 0))
    down_cy = core(jnp.concatenate([down_y[hid:], down_y[:hid]], 0))
    down_all = jnp.concatenate(
        [jnp.concatenate([down[0], down[1]], 0), down_c, down_y, down_cy], axis=1
    )

    experts = jnp.arange(sp_count, dtype=jnp.int32)
    table = jnp.sum(
        jnp.where(route_ids[None] == experts[:, None, None], route_weight[None], 0.0), axis=2
    )
    parts = pieces(table, 1)
    sent = jnp.concatenate([parts[0], parts[2]], axis=1)
    arrived = lax.all_to_all(sent, "sp", split_axis=0, concat_axis=0, tiled=True)

    mixer = jnp.concatenate(
        [(p) for p in pieces(mixed_rows(pre_gate, value_in, post_gate, conv_taps))], 0
    ).reshape(tp_count, own_rows, -1)
    away = jnp.dot(
        jnp.concatenate([mixer[1], mixer[3]], 0), out_weight, preferred_element_type=f32
    ).astype(bf16)
    back = core(away)
    kept = jnp.dot(
        jnp.concatenate([mixer[0], mixer[2]], 0), out_weight, preferred_element_type=f32
    ) + back.astype(f32)
    from_y = along_y(kept[own_rows:].astype(bf16))
    residual = (stream_in.astype(f32) + kept[:own_rows] + from_y.astype(f32)).astype(bf16)
    normed = scaled_norm(residual.astype(f32), ffn_gain).astype(bf16)

    planes = sp_count // 2
    own = [normed] + [swap(normed, 2 * k, 0) for k in range(1, planes)]
    sums = []
    for k in range(planes):
        at_x = along_x(own[k])
        at_y = along_y(own[k])
        diag = jnp.concatenate([along_y(at_x[:half]), along_x(at_y[half:])], 0)
        rows = jnp.concatenate([own[k], at_x, at_y, diag], 0)
        h_own = clamped_units(
            jnp.dot(rows, gate_own, preferred_element_type=f32),
            jnp.dot(rows, up_own, preferred_element_type=f32),
        ).astype(bf16)
        h_other = clamped_units(
            jnp.dot(rows, gate_other, preferred_element_type=f32),
            jnp.dot(rows, up_other, preferred_element_type=f32),
        ).astype(bf16)
        at_own = lax.dynamic_index_in_dim(arrived, sp_index ^ (2 * k), 0, False)
        at_near = lax.dynamic_index_in_dim(arrived, sp_index ^ (2 * k + 1), 0, False)
        scale = jnp.concatenate(
            [at_own[:own_rows], at_near[:own_rows], at_own[own_rows:], at_near[own_rows:]]
        )
        out = jnp.dot(
            jnp.concatenate([h_own, h_other], axis=1), down_all, preferred_element_type=f32
        )
        out = (out * scale[:, None]).astype(bf16).reshape(4, own_rows, width)
        by_y = y_turned(along_y(out[3, :half]))
        by_x = along_x(out[3, half:])
        for_x = jnp.concatenate(
            [(out[1, :half].astype(f32) + by_y.astype(f32)).astype(bf16), out[1, half:]], 0
        )
        for_y = jnp.concatenate(
            [out[2, :half], (out[2, half:].astype(f32) + by_x.astype(f32)).astype(bf16)], 0
        )
        total = (
            out[0].astype(f32)
            + along_x(for_x).astype(f32)
            + y_turned(along_y(for_y)).astype(f32)
        )
        sums.append(total if k == 0 else swap(total.astype(bf16), 2 * k, 0).astype(f32))
    total = sum(sums)
    quarters = jnp.split(total, tp_count, axis=1)
    flip_c, flip_y = (tp_index & 1) == 1, (tp_index & 2) == 2
    turned = [jnp.where(flip_c, quarters[j ^ 1], quarters[j]) for j in range(tp_count)]
    turned = [jnp.where(flip_y, turned[j ^ 2], turned[j]) for j in range(tp_count)]
    combined = jnp.concatenate(turned, axis=1).astype(bf16)
    layer_out = residual.astype(f32) + scaled_norm(combined.astype(f32), post_gain)
    return layer_out.astype(bf16)


def local(*arrays):
    sp_count = lax.axis_size("sp")
    tp_count = lax.axis_size("tp")
    seq_rows = arrays[1].shape[0]
    own_rows = seq_rows // tp_count
    slots_each = 2 * own_rows * arrays[6].shape[1] // sp_count
    plain = slots_each >= own_rows and tp_count == 4 and sp_count >= 2
    plain = plain and sp_count & (sp_count - 1) == 0 and arrays[10].shape[0] == 1
    return (dense if plain else slotted)(*arrays)


def solution(mesh):
    placed = (
        P(("sp", "tp"), None),
        P("sp", "tp"),
        P("sp", "tp"),
        P("sp", "tp"),
        P(None, "tp"),
        P("tp", None),
        P("sp", None),
        P("sp", None),
        P(),
        P(),
        P("sp", None, "tp"),
        P("sp", None, "tp"),
        P("sp", None, "tp"),
    )
    return jax.shard_map(
        local, mesh=mesh, in_specs=placed, out_specs=P(("sp", "tp"), None), check_vma=False
    )
```
